32 devices in a mesh: ep: 8 (over z, x), tp: 4 (over y, core).
Axes of the slice: x: 2, y: 2, z: 4, core: 2. Of those that a mesh axis runs over, the one named last changes fastest.
Arguments:
- tokens: bfloat16 [256, 4096], P('ep'), may hold values from -6 to 6
- routes: int32 [256, 4], P('ep'), may hold values from 0 to 7, all different within a row; in each aligned block of 32 rows (0 to 31, 32 to 63, ...) at most 24 rows name the same one
- mix_weights: float32 [256, 4], P('ep'), may hold values from 0.2 to 1
- pre_gain: float32 [4096], replicated, may hold values from 0.1 to 1.9
- gate_weight: bfloat16 [8, 4096, 2048], P('ep', None, 'tp'), may hold values from -0.09375 to 0.09375
- up_weight: bfloat16 [8, 4096, 2048], P('ep', None, 'tp'), may hold values from -0.09375 to 0.09375
- down_weight: bfloat16 [8, 2048, 4096], P('ep', 'tp'), may hold values from -1 to 1
- post_gain: float32 [4096], P('tp'), may hold values from 0.1 to 1.9
Outputs:
- layer_out: bfloat16 [256, 4096], P('ep', 'tp')
The draws below stay inside these ranges and needn't reach their ends.
Inputs may be any that keep to these rules, and one draw needn't show every extreme that they name: `routes`: within a row the 4 experts differ; among the rows of one index of ep no expert is named more than 24 times.
All inputs are finite; a program needn't handle non-finite values.
Results may differ from the reference program's by a relative error of at most 0.019.
Values may be sent and summed in bfloat16 or wider, within the bound.
No kernel may reach another device: no remote copies, remote signals or barrier semaphores. Data moves between devices by JAX's collectives and lax.ppermute only.
A program may use at most 64 MiB of HBM per device.

```python
import math
import jax
import jax.numpy as jnp
import numpy as np
from jax import lax

D = 4096
FF = 2048
TOP = 4
TOK_DEV = 32
EXPERTS = 8
CAP = 24
TOKENS = 256
N_EP = 8
N_TP = 4


def draw_down_weight(key, part):
    noise = jnp.clip(jax.random.normal(jax.random.fold_in(key, 11), (EXPERTS, FF, D), jnp.float32), -6.0, 6.0)
    noise = noise * FF ** (-0.5)
    position = jnp.arange(D, dtype=jnp.float32) / D
    rise = 3.0 ** position * jax.random.uniform(jax.random.fold_in(key, 12), (D,), jnp.float32, 0.6, 1.6)
    return jnp.clip(noise * rise, -1.0, 1.0).astype(jnp.bfloat16)


def steps_of(key, shape, split, smallest, high):
    loudness = 1.0
    for axis_at, parts in split:
        steps = jax.random.uniform(jax.random.fold_in(jax.random.fold_in(key, 6), axis_at), (parts,), jnp.float32, smallest / len(split), high / len(split))
        loudness = loudness * jnp.repeat(jnp.exp(steps), shape[axis_at] // parts).reshape((-1,) + (1,) * (len(shape) - 1 - axis_at))
    return loudness


def assign_block(rng, own, number, rows, amount, top, most, skew):
    order = jax.random.permutation(rng, amount)
    packed, ordinary = portions_of(amount, rows * top, most, skew, True), portions_of(amount, rows * top, most, skew, False)
    places = jnp.arange(amount)

    def named(lengths, offset_by):
        used = int((lengths > 0).sum())
        fixed = max(1, used // 4)
        shifted = fixed + (places - fixed + offset_by * (used - fixed)) % max(1, amount - fixed)
        return jnp.zeros((amount,), jnp.int32).at[order[jnp.where(places < fixed, places, shifted)]].set(jnp.asarray(lengths, jnp.int32))

    lengths = jnp.where(number % 4 == 0, named(packed, number // 4), named(ordinary, number - number // 4 - 1))
    mixed = jax.random.permutation(jax.random.fold_in(own, 3), amount)
    giver, taker = mixed[0:amount // 2 * 2:2], mixed[1:amount // 2 * 2:2]
    margin = jnp.minimum(lengths[giver] - 1, most - lengths[taker]) // 2
    margin = jnp.where((giver == order[0]) | (taker == order[0]) | (lengths[taker] == 0), 0, jnp.maximum(margin, 0))
    shifted = jax.random.randint(jax.random.fold_in(own, 4), (amount // 2,), 0, 1 << 20) % (margin + 1)
    lengths = lengths.at[giver].add(-shifted).at[taker].add(shifted)
    labels = jnp.searchsorted(jnp.cumsum(lengths), jnp.arange(rows * top), side="right").astype(jnp.int32)
    grid = labels.reshape(top, rows).T
    grid = grid[jax.random.permutation(jax.random.fold_in(own, 1), rows)]
    offset_by = jax.random.randint(jax.random.fold_in(own, 2), (rows, 1), 0, top)
    return jnp.take_along_axis(grid, (jnp.arange(top)[None, :] + offset_by) % top, axis=1)


def portions_of(amount, total, limit, lean, full):
    portions = [(1 << 20) // math.isqrt(rank ** lean) + 1 for rank in range(1, amount + 1)]
    largest = limit if full else min(limit, max(-(-total // amount), total * portions[0] // sum(portions)))
    least = 1 if total - largest >= amount - 1 else 0
    given, surplus = [largest] + [least] * (amount - 1), total - largest - least * (amount - 1)
    while surplus > 0:
        free = [i for i in range(1, amount) if given[i] < largest] or [i for i in range(1, amount) if given[i] < limit]
        mass, left = sum([portions[i] for i in free]), surplus
        for i in free:
            extra = min(limit - given[i], max(1, left * portions[i] // mass), surplus)
            given[i] = given[i] + extra
            surplus = surplus - extra
    return np.array(given)


def bell_draw(own_key, extent, deviation, most, split=(), kind=jnp.bfloat16):
    level = steps_of(own_key, extent, split, -0.22, 0.18) if split else 1.0
    values = jax.random.normal(own_key, extent, jnp.float32) * deviation * level
    return jnp.minimum(jnp.maximum(values, -most), most).astype(kind)


def setup_inputs(seed: int = 0) -> dict:
    streams_of = jax.random.split(jax.random.key(seed), 9)
    tokens = bell_draw(streams_of[0], (TOKENS, D), 1.0, 6.0, ((0, 8),))
    routes_keys = jax.random.split(jax.random.fold_in(streams_of[1], 1), TOKENS // TOK_DEV)
    routes_turns = jax.random.permutation(jax.random.fold_in(streams_of[1], 3), TOKENS // TOK_DEV)
    routes = jax.vmap(lambda own, number: assign_block(jax.random.fold_in(streams_of[1], 2), own, number, TOK_DEV, EXPERTS, TOP, CAP, 2))(routes_keys, routes_turns).reshape((TOKENS, TOP))
    mix_weights = jnp.clip(0.2 + 0.8 * jax.random.uniform(streams_of[2], (TOKENS, TOP), jnp.float32) ** steps_of(streams_of[2], (TOKENS, TOP), ((0, 8),), -0.2, 0.2), 0.2, 1.0)
    pre_gain = jnp.clip(1.0 + 0.18 * jax.random.normal(streams_of[3], (D,), jnp.float32), 0.1, 1.9)
    gate_weight = bell_draw(streams_of[4], (EXPERTS, D, FF), D ** -0.5, 0.09375, ((0, 8), (2, 4)))
    up_weight = bell_draw(streams_of[5], (EXPERTS, D, FF), D ** -0.5, 0.09375, ((0, 8), (2, 4)))
    down_weight = draw_down_weight(jax.random.fold_in(streams_of[8], 71), 0)
    post_gain = jnp.clip(1.0 + 0.18 * jax.random.normal(streams_of[7], (D,), jnp.float32), 0.1, 1.9)
    return dict(tokens=tokens, routes=routes, mix_weights=mix_weights, pre_gain=pre_gain, gate_weight=gate_weight, up_weight=up_weight, down_weight=down_weight, post_gain=post_gain)


epsilon = 1e-06

def reference(tokens, routes, mix_weights, pre_gain, gate_weight, up_weight, down_weight, post_gain):
    floats = tokens.astype(jnp.float32)
    normed = (floats * lax.rsqrt(lax.optimization_barrier(jnp.mean(floats * floats, axis=-1, keepdims=True)) + epsilon) * pre_gain).astype(jnp.bfloat16)
    row_slots = N_EP * CAP
    group_width = FF // N_TP

    def visit_expert(result, per_expert):
        w_gate, w_up, w_down, expert_id = per_expert
        matches = routes == expert_id
        weight = lax.optimization_barrier(jnp.sum(jnp.where(matches, mix_weights, 0.0), axis=1))
        is_named = jnp.any(matches, axis=1)
        row_index = jnp.nonzero(is_named, size=row_slots, fill_value=0)[0].astype(jnp.int32)
        is_live = jnp.arange(row_slots) < jnp.sum(is_named.astype(jnp.int32))
        picked = normed[row_index]
        gate_act = jnp.dot(picked, w_gate, preferred_element_type=jnp.float32)
        up_act = jnp.dot(picked, w_up, preferred_element_type=jnp.float32)
        hidden = (jax.nn.silu(gate_act) * up_act).astype(jnp.bfloat16)
        pieces = jnp.einsum('rgf,gfd->grd', hidden.reshape(row_slots, N_TP, group_width).astype(jnp.float32), w_down.reshape(N_TP, group_width, D).astype(jnp.float32))
        pieces = lax.optimization_barrier(pieces.astype(jnp.bfloat16)).astype(jnp.float32)
        expert_out = lax.optimization_barrier(lax.optimization_barrier(jnp.sum(pieces, axis=0)).astype(jnp.bfloat16)).astype(jnp.float32)
        weighting = jnp.where(is_live, weight[row_index], 0.0)
        result = result.at[row_index].add(weighting[:, None] * expert_out)
        return (result, None)
    start = jnp.zeros((tokens.shape[0], D), jnp.float32)
    mixed, _ = lax.scan(visit_expert, start, (gate_weight, up_weight, down_weight, jnp.arange(EXPERTS, dtype=jnp.int32)))
    scale = lax.rsqrt(lax.optimization_barrier(jnp.mean(mixed * mixed, axis=-1, keepdims=True)) + epsilon)
    return (mixed * scale * post_gain).astype(jnp.bfloat16)
```

```python
import jax
import jax.numpy as jnp
from jax import lax
from jax.sharding import PartitionSpec as P

epsilon = 1e-06
direct_limit = 16


def send(value, axis, move):
    size = lax.axis_size(axis)
    return lax.ppermute(value, axis, [(i, move(i, size)) for i in range(size)])


def on_device(
    tokens, routes, mix_weights, pre_gain, gate_weight, up_weight, down_weight, post_gain
):
    tok_rows, width = tokens.shape
    top_count = routes.shape[1]
    experts = lax.axis_size("ep")
    shards = lax.axis_size("tp")
    chips = shards // 2
    piece = width // shards
    half = width // 2
    direct = experts <= direct_limit
    capacity = min(tok_rows, max(2, (3 * tok_rows * top_count + 2 * experts - 1) // (2 * experts)))
    slots = experts * capacity
    core = lax.axis_index("tp") % 2
    chip = lax.axis_index("tp") // 2

    def exchange(rows, back):
        if not direct:
            blocks = rows.reshape(experts, capacity, rows.shape[1])
            blocks = lax.all_to_all(blocks, "ep", split_axis=0, concat_axis=0, tiled=True)
            return blocks.reshape(rows.shape)
        sign = -1 if back else 1
        parts = [rows[:capacity]]
        for k in range(1, experts):
            block = rows[k * capacity : (k + 1) * capacity]
            parts.append(send(block, "ep", lambda i, n, k=k: (i + sign * k) % n))
        return jnp.concatenate(parts, axis=0)

    chosen = routes.reshape(-1)
    if direct:
        chosen = (chosen - lax.axis_index("ep")) % experts
    onehot = (chosen[:, None] == jnp.arange(experts, dtype=jnp.int32)[None, :]).astype(jnp.float32)
    count = tok_rows * top_count
    earlier = (
        jnp.arange(count, dtype=jnp.int32)[:, None] > jnp.arange(count, dtype=jnp.int32)[None, :]
    ).astype(jnp.float32)
    before = jnp.dot(earlier, onehot, preferred_element_type=jnp.float32)
    slot_rank = jnp.sum(before * onehot, axis=1).astype(jnp.int32)
    target = (chosen * capacity + slot_rank).reshape(tok_rows, top_count)
    by_choice = target[:, :, None] == jnp.arange(slots, dtype=jnp.int32)[None, None, :]
    picked = jnp.any(by_choice, axis=1).astype(jnp.bfloat16)
    mixing = jnp.sum(jnp.where(by_choice, mix_weights[:, :, None], 0.0), axis=1)

    floats = tokens.astype(jnp.float32)
    scale = lax.rsqrt(jnp.mean(floats * floats, axis=-1, keepdims=True) + epsilon)
    own_half = lax.dynamic_slice_in_dim(tokens, core * half, half, 1).astype(jnp.float32)
    own_gain = lax.dynamic_slice_in_dim(pre_gain, core * half, half, 0)
    normed = (own_half * scale * own_gain).astype(jnp.bfloat16)
    outgoing = jnp.dot(picked.T, normed, preferred_element_type=jnp.float32).astype(jnp.bfloat16)
    mine = exchange(outgoing, False)
    other = send(mine, "tp", lambda i, n: i ^ 1)
    is_first = core == 0
    arrived = jnp.concatenate(
        [jnp.where(is_first, mine, other), jnp.where(is_first, other, mine)], axis=1
    )
    gate_act = jnp.dot(arrived, gate_weight[0], preferred_element_type=jnp.float32)
    up_act = jnp.dot(arrived, up_weight[0], preferred_element_type=jnp.float32)
    hidden = (jax.nn.silu(gate_act) * up_act).astype(jnp.bfloat16)
    partial_value = jnp.dot(hidden, down_weight[0], preferred_element_type=jnp.float32)
    partial_value = partial_value.astype(jnp.bfloat16)
    firsts = jnp.concatenate(
        [partial_value[:, (2 * j) * piece : (2 * j + 1) * piece] for j in range(chips)], axis=1
    )
    seconds = jnp.concatenate(
        [partial_value[:, (2 * j + 1) * piece : (2 * j + 2) * piece] for j in range(chips)], axis=1
    )
    kept = jnp.where(is_first, firsts, seconds)
    given = jnp.where(is_first, seconds, firsts)
    gained = send(given, "tp", lambda i, n: i ^ 1)
    chip_sum = (kept.astype(jnp.float32) + gained.astype(jnp.float32)).astype(jnp.bfloat16)
    returned = exchange(chip_sum, True)
    mixed_part = jnp.dot(mixing, returned.astype(jnp.float32), precision=lax.Precision.HIGHEST)
    mixed_sent = mixed_part.astype(jnp.bfloat16)
    mixed = mixed_part
    for k in range(1, chips):
        mixed = mixed + send(mixed_sent, "tp", lambda i, n, k=k: (i + 2 * k) % n).astype(jnp.float32)
    squares = jnp.sum(mixed * mixed, axis=1, keepdims=True)
    squares = jnp.broadcast_to(squares, (tok_rows, 128))
    total = squares + send(squares, "tp", lambda i, n: i ^ 1)
    scale_out = lax.rsqrt(total[:, :1] / width + epsilon)
    result = lax.dynamic_slice_in_dim(mixed, chip * piece, piece, 1)
    return (result * scale_out * post_gain).astype(jnp.bfloat16)


def solution(mesh):
    in_specs = (
        P("ep", None),
        P("ep", None),
        P("ep", None),
        P(),
        P("ep", None, "tp"),
        P("ep", None, "tp"),
        P("ep", "tp", None),
        P("tp"),
    )
    out_specs = P("ep", "tp")
    return jax.shard_map(
        on_device, mesh=mesh, in_specs=in_specs, out_specs=out_specs, check_vma=False
    )
```

```python
import jax
import jax.numpy as jnp
from jax import lax
from jax.experimental import pallas as pl
from jax.experimental.pallas import tpu as pltpu
from jax.sharding import PartitionSpec as P

epsilon = 1e-06
direct_limit = 16


def send(value, axis, move):
    size = lax.axis_size(axis)
    return lax.ppermute(value, axis, [(i, move(i, size)) for i in range(size)])


def start_all(pairs, sems):
    copies = [pltpu.make_async_copy(src, dst, sems.at[i]) for i, (src, dst) in enumerate(pairs)]
    for copy in copies:
        copy.start()
    return copies


def select_body(core_ref, picked, gain, tokens_hbm, outgoing, token_buf, sems):
    half = token_buf.shape[2]
    copies = start_all(
        [(tokens_hbm.at[:, pl.ds(j * half, half)], token_buf.at[j]) for j in range(2)], sems
    )
    total = 0.0
    for j in range(2):
        copies[j].wait()
        floats = token_buf[j].astype(jnp.float32)
        total = total + jnp.sum(floats * floats, axis=1, keepdims=True)
    scale = lax.rsqrt(total / (2 * half) + epsilon)
    core = core_ref[0]
    own_gain = gain[pl.ds(core, 1), :]
    normed = (token_buf[core].astype(jnp.float32) * scale * own_gain).astype(jnp.bfloat16)
    outgoing[...] = lax.dot_general(
        picked[...], normed, (((0,), (0,)), ((), ())), preferred_element_type=jnp.float32
    ).astype(jnp.bfloat16)


def half_products(part, rows_hbm, gate_hbm, up_hbm, rows_buf, gate_buf, up_buf, sems, extra):
    half = rows_buf.shape[1]
    steps, chunk = gate_buf.shape[0], gate_buf.shape[1]
    pairs = [(rows_hbm, rows_buf)]
    for j in range(steps):
        rows = pl.ds(pl.multiple_of(part * half + j * chunk, chunk), chunk)
        pairs.append((gate_hbm.at[0, rows, :], gate_buf.at[j]))
        pairs.append((up_hbm.at[0, rows, :], up_buf.at[j]))
    copies = start_all(pairs + extra, sems)
    copies[0].wait()
    gate_act = up_act = 0.0
    for j in range(steps):
        rows = rows_buf[:, j * chunk : (j + 1) * chunk]
        copies[2 * j + 1].wait()
        gate_act = gate_act + jnp.dot(rows, gate_buf[j], preferred_element_type=jnp.float32)
        copies[2 * j + 2].wait()
        up_act = up_act + jnp.dot(rows, up_buf[j], preferred_element_type=jnp.float32)
    return gate_act, up_act, copies[2 * steps + 1 :]


def first_body(core_ref, rows_hbm, gate_hbm, up_hbm, gate_out, up_out, rows_buf, gate_buf, up_buf, sems):
    gate_out[...], up_out[...], _ = half_products(
        core_ref[0], rows_hbm, gate_hbm, up_hbm, rows_buf, gate_buf, up_buf, sems, []
    )


def down_pairs(part, down_hbm, down_buf):
    chips, piece = down_buf.shape[0], down_buf.shape[2]
    pairs = []
    for p in range(chips):
        start = pl.multiple_of((2 * p + part) * piece, piece)
        pairs.append((down_hbm.at[0, :, pl.ds(start, piece)], down_buf.at[p]))
    return pairs


def down_products(hidden, copies, down_buf, target):
    chips, piece = down_buf.shape[0], down_buf.shape[2]
    for p in range(chips):
        copies[p].wait()
        value = jnp.dot(hidden, down_buf[p], preferred_element_type=jnp.float32)
        target[:, p * piece : (p + 1) * piece] = value.astype(jnp.bfloat16)


def second_body(
    core_ref, gate_first, up_first, rows_hbm, gate_hbm, up_hbm, down_hbm, hidden_out, given,
    rows_buf, gate_buf, up_buf, down_buf, sems,
):
    other = 1 - core_ref[0]
    gate_act, up_act, copies = half_products(
        other, rows_hbm, gate_hbm, up_hbm, rows_buf, gate_buf, up_buf, sems,
        down_pairs(other, down_hbm, down_buf),
    )
    gate_act = gate_act + gate_first[...]
    up_act = up_act + up_first[...]
    hidden = (gate_act / (1.0 + jnp.exp(-gate_act)) * up_act).astype(jnp.bfloat16)
    hidden_out[...] = hidden
    down_products(hidden, copies, down_buf, given)


def third_body(core_ref, hidden, down_hbm, kept, down_buf, sems):
    copies = start_all(down_pairs(core_ref[0], down_hbm, down_buf), sems)
    down_products(hidden[...], copies, down_buf, kept)


smem = pl.BlockSpec(memory_space=pltpu.SMEM)
vmem = pl.BlockSpec(memory_space=pltpu.VMEM)
hbm = pl.BlockSpec(memory_space=pltpu.MemorySpace.HBM)


def in_hbm(value):
    return pltpu.with_memory_space_constraint(value, pltpu.MemorySpace.HBM)


def on_core(body, name, shapes, specs, scratch, copies):
    return pl.pallas_call(
        body,
        out_shape=tuple(jax.ShapeDtypeStruct(*shape) for shape in shapes),
        in_specs=[smem] + specs,
        out_specs=tuple(vmem for _ in shapes),
        scratch_shapes=[pltpu.VMEM(shape, jnp.bfloat16) for shape in scratch]
        + [pltpu.SemaphoreType.DMA((copies,))],
        compiler_params=pltpu.CompilerParams(vmem_limit_bytes=32 * 1024 * 1024),
        name=name,
    )


def run_expert(core, mine, gate_weight, up_weight, down_weight, piece):
    slots, half = mine.shape
    units = gate_weight.shape[2]
    chips = down_weight.shape[2] // (2 * piece)
    gate_weight, up_weight, down_weight = map(in_hbm, (gate_weight, up_weight, down_weight))
    steps = 2
    chunk = half // steps
    halves = [(slots, half), (steps, chunk, units), (steps, chunk, units)]
    downs = (chips, units, piece)
    acts = ((slots, units), jnp.float32)
    wide = ((slots, half), jnp.bfloat16)
    where = core.reshape(1).astype(jnp.int32)
    other = send(mine, "tp", lambda i, n: i ^ 1)
    gate_first, up_first = on_core(
        first_body, "first", (acts, acts), [hbm] * 3, halves, 2 * steps + 1
    )(where, mine, gate_weight, up_weight)
    hidden, given = on_core(
        second_body, "second", (((slots, units), jnp.bfloat16), wide), [vmem] * 2 + [hbm] * 4,
        halves + [downs], 2 * steps + 1 + chips,
    )(where, gate_first, up_first, other, gate_weight, up_weight, down_weight)
    gained = send(given, "tp", lambda i, n: i ^ 1)
    (kept,) = on_core(third_body, "third", (wide,), [vmem, hbm], [downs], chips)(
        where, hidden, down_weight
    )
    return kept, gained


def on_device(
    tokens, routes, mix_weights, pre_gain, gate_weight, up_weight, down_weight, post_gain
):
    tok_rows, width = tokens.shape
    top_count = routes.shape[1]
    experts = lax.axis_size("ep")
    shards = lax.axis_size("tp")
    chips = shards // 2
    piece = width // shards
    half = width // 2
    paired = False
    order = list(range(experts - 1, 0, -1))
    direct = experts <= direct_limit
    capacity = min(tok_rows, max(2, (3 * tok_rows * top_count + 2 * experts - 1) // (2 * experts)))
    slots = experts * capacity
    core = lax.axis_index("tp") % 2
    chip = lax.axis_index("tp") // 2

    def exchange(rows, back):
        if not direct:
            blocks = rows.reshape(experts, capacity, rows.shape[1])
            blocks = lax.all_to_all(blocks, "ep", split_axis=0, concat_axis=0, tiled=True)
            return blocks.reshape(rows.shape)
        sign = -1 if back else 1
        parts = {0: rows[:capacity]}
        for k in order:
            block = rows[k * capacity : (k + 1) * capacity]
            if paired:
                parts[k] = send(block, "ep", lambda i, n, k=k: i ^ k)
            else:
                parts[k] = send(block, "ep", lambda i, n, k=k: (i + sign * k) % n)
        return jnp.concatenate([parts[k] for k in range(experts)], axis=0)

    chosen = routes.reshape(-1)
    if direct:
        here = lax.axis_index("ep")
        chosen = chosen ^ here if paired else (chosen - here) % experts
    onehot = (chosen[:, None] == jnp.arange(experts, dtype=jnp.int32)[None, :]).astype(jnp.float32)
    count = tok_rows * top_count
    earlier = (
        jnp.arange(count, dtype=jnp.int32)[:, None] > jnp.arange(count, dtype=jnp.int32)[None, :]
    ).astype(jnp.float32)
    before = jnp.dot(earlier, onehot, preferred_element_type=jnp.float32)
    slot_rank = jnp.sum(before * onehot, axis=1).astype(jnp.int32)
    target = (chosen * capacity + slot_rank).reshape(tok_rows, top_count)
    by_choice = target[:, :, None] == jnp.arange(slots, dtype=jnp.int32)[None, None, :]
    picked = jnp.any(by_choice, axis=1).astype(jnp.bfloat16)
    mixing = jnp.sum(jnp.where(by_choice, mix_weights[:, :, None], 0.0), axis=1)

    (outgoing,) = on_core(
        select_body, "select", (((slots, half), jnp.bfloat16),), [vmem, vmem, hbm],
        [(2, tok_rows, half)], 2,
    )(core.reshape(1).astype(jnp.int32), picked, pre_gain.reshape(2, half), in_hbm(tokens))
    mine = exchange(outgoing, False)
    kept, gained = run_expert(core, mine, gate_weight, up_weight, down_weight, piece)
    chip_sum = (kept.astype(jnp.float32) + gained.astype(jnp.float32)).astype(jnp.bfloat16)
    returned = exchange(chip_sum, True)
    mixed_part = jnp.dot(mixing, returned.astype(jnp.float32), precision=lax.Precision.HIGHEST)
    mixed_sent = mixed_part.astype(jnp.bfloat16)
    mixed = mixed_part
    for k in range(1, chips):
        mixed = mixed + send(mixed_sent, "tp", lambda i, n, k=k: (i + 2 * k) % n).astype(jnp.float32)
    squares = jnp.sum(mixed * mixed, axis=1, keepdims=True)
    squares = jnp.broadcast_to(squares, (tok_rows, 128))
    total = squares + send(squares, "tp", lambda i, n: i ^ 1)
    scale_out = lax.rsqrt(total[:, :1] / width + epsilon)
    result = lax.dynamic_slice_in_dim(mixed, chip * piece, piece, 1)
    return (result * scale_out * post_gain).astype(jnp.bfloat16)


def solution(mesh):
    in_specs = (
        P("ep", None),
        P("ep", None),
        P("ep", None),
        P(),
        P("ep", None, "tp"),
        P("ep", None, "tp"),
        P("ep", "tp", None),
        P("tp"),
    )
    out_specs = P("ep", "tp")
    return jax.shard_map(
        on_device, mesh=mesh, in_specs=in_specs, out_specs=out_specs, check_vma=False
    )
```
